32 devices in a mesh: sp: 16 (over z, y, x), tp: 2 (over core).
Axes of the slice: x: 2, y: 2, z: 4, core: 2. Of those that a mesh axis runs over, the one named last changes fastest.
Arguments:
- skip_path_inputs: bfloat16 [2048, 2048], P('sp'), may hold values from -62 to 62
- probe_vectors: bfloat16 [2048, 1024], P('sp', 'tp'), may hold values from -6 to 6
- lookup_vectors: bfloat16 [2048, 1024], P('sp', 'tp'), may hold values from -6 to 6
- payload_vectors: bfloat16 [2048, 1024], P('sp', 'tp'), may hold values from -6 to 6
- learning_strength_preacts: float32 [2, 2048, 8], P(None, 'sp', 'tp'), may hold values from -6 to 6
- forget_preacts: float32 [2, 2048, 8], P(None, 'sp', 'tp'), may hold values from -5 to 5
- forgetting_speed_exponent: float32 [2, 8], P(None, 'tp'), may hold values from -12 to -2
- extra_forgetting_spikes: float32 [2, 2048, 8], P(None, 'sp', 'tp'), may hold values from -0.7 to 0
- sample_membership: int32 [2048], P('sp'), may hold values from 0 to 3, never falling along the last dimension, each value on 1 to 1024 neighbouring positions
- channel_group_scaling: float32 [128], replicated, may hold values from 0.1 to 1.9
- blend_exit_weights: bfloat16 [1024, 2048], P('tp'), may hold values from -0.1875 to 0.1875
- dense_block_scaling: float32 [2048], replicated, may hold values from 0.1 to 1.9
- widen_projection_weights: bfloat16 [2048, 8192], P('sp', 'tp'), may hold values from -0.125 to 0.125
- shrink_projection_weights: bfloat16 [8192, 2048], P('tp', 'sp'), may hold values from -0.0625 to 0.0625
Outputs:
- result: bfloat16 [2048, 2048], P('sp', 'tp')
The draws below stay inside these ranges and needn't reach their ends.
Inputs may be any that keep to these rules, and one draw needn't show every extreme that they name: `sample_membership`: document numbers never fall along the positions; each document holds 1 to 1024 positions.
All inputs are finite; a program needn't handle non-finite values.
Results may differ from the reference program's by a relative error of at most 0.015.
Values may be sent and summed in bfloat16 or wider, within the bound.
A program may use at most 128 MiB of HBM per device.

```python
import math
import jax
import jax.numpy as jnp
import numpy as np
from jax import lax

D = 2048
HEADS = 8
HEAD = 128
FF = 8192
BLOCK = 64
TOK_DEV = 128
TOKENS = 2048
DOCS = 4
DOC_MOST = 1024
N_TP = 2


def draw_skip_path_inputs(key, part):
    pieces = jax.random.split(key, 2)
    base = jnp.clip(jax.random.normal(pieces[0], (TOKENS, D), jnp.float32), -5.0, 5.0)
    ramp = jnp.exp(math.log(3.0) * (jnp.arange(D, dtype=jnp.float32) / D - 0.5))
    jitter = jnp.exp(jax.random.uniform(pieces[1], (D,), jnp.float32, -1.15, 1.15))
    return (base * ramp * jitter).astype(jnp.bfloat16)


def draw_forgetting_speed_exponent(key, part):
    pieces = jax.random.split(key, 3)
    share = 0.5
    quick_pick = jax.random.uniform(pieces[0], (2, HEADS), jnp.float32) < share
    quick = math.log(math.log(10.0) / 50.0) + jax.random.uniform(pieces[1], (2, HEADS), jnp.float32, math.log(0.6), math.log(1.6))
    gentle = math.log(math.log(10.0) / (8 * TOK_DEV)) + jax.random.uniform(pieces[2], (2, HEADS), jnp.float32, math.log(0.2), 0.0)
    return jnp.where(quick_pick, quick, gentle).astype(jnp.float32)


def draw_forget_preacts(key, part):
    pieces = jax.random.split(key, 2)
    block_count = TOKENS // TOK_DEV
    offset = jax.random.uniform(pieces[0], (2, block_count, 1, HEADS), jnp.float32, -1.2, 1.2)
    noise = 0.6 * jnp.clip(jax.random.normal(pieces[1], (2, block_count, TOK_DEV, HEADS), jnp.float32), -6.0, 6.0)
    return (noise + offset).reshape(2, TOKENS, HEADS).astype(jnp.float32)


def draw_extra_forgetting_spikes(key, part):
    pieces = jax.random.split(key, 2)
    struck = jax.random.bernoulli(pieces[0], 1.0 / (2 * TOK_DEV), (2, TOKENS, HEADS))
    depth = jnp.log(jax.random.uniform(pieces[1], (2, TOKENS, HEADS), jnp.float32, 0.5, 0.8))
    return jnp.where(struck, depth, 0.0).astype(jnp.float32)


def steps_of(stream_key, shape, cuts, smallest, largest):
    def one(axis_at, shards_of):
        steps = jax.random.uniform(jax.random.fold_in(jax.random.fold_in(stream_key, 6), axis_at), (shards_of,), jnp.float32, smallest / len(cuts), largest / len(cuts))
        return jnp.repeat(jnp.exp(steps), shape[axis_at] // shards_of).reshape((-1,) + (1,) * (len(shape) - axis_at - 1))

    level = one(*cuts[0])
    for cut in cuts[1:]:
        level = level * one(*cut)
    return level


def profile(count, total, limit, slope):
    weights = [(1 << 20) // math.isqrt(grade ** slope) + 1 for grade in range(2, count + 1)]
    surplus, given = total - limit - (count - 1), [1] * (count - 1)
    while surplus > 0:
        free = [i for i in range(count - 1) if given[i] < limit]
        pool, budget = sum([weights[i] for i in free]), surplus
        for i in free:
            more = min(limit - given[i], max(1, budget * weights[i] // pool), surplus)
            given[i] = given[i] + more
            surplus = surplus - more
    return np.array([limit] + given)


def ragged_sizes(rng, count, total, reach, slope):
    if count == 2:
        one = jax.random.randint(rng, (), max(1, total - reach), min(reach, total - 1) + 1)
        return jnp.stack([one, total - one])
    sizes = jnp.asarray(profile(count, total, reach, slope), jnp.int32)
    twos = (count - 1) // 2
    source_of, receiver = sizes[1:1 + 2 * twos:2], sizes[2:2 + 2 * twos:2]
    room = jnp.minimum(source_of - 1, reach - receiver)
    moved = jax.random.randint(jax.random.fold_in(rng, 1), (twos,), 0, 1 << 20) % (room + 1)
    sizes = sizes.at[1:1 + 2 * twos:2].set(source_of - moved).at[2:2 + 2 * twos:2].set(receiver + moved)
    return sizes[jax.random.permutation(jax.random.fold_in(rng, 2), count)]


def centred(own_key, shape, width, most, shards=(), kind=jnp.bfloat16):
    level = steps_of(own_key, shape, shards, -0.22, 0.18) if shards else 1.0
    entries = jax.random.normal(own_key, shape, jnp.float32) * width * level
    return jnp.minimum(jnp.maximum(entries, -most), most).astype(kind)


def setup_inputs(seed: int = 0) -> dict:
    splits = jax.random.split(jax.random.key(seed), 15)
    skip_path_inputs = draw_skip_path_inputs(jax.random.fold_in(splits[14], 71), 0)
    probe_vectors = centred(splits[1], (TOKENS, HEADS * HEAD), 1.0, 6.0, ((0, 16), (1, 2)))
    lookup_vectors = centred(splits[2], (TOKENS, HEADS * HEAD), 1.0, 6.0, ((0, 16), (1, 2)))
    payload_vectors = centred(splits[3], (TOKENS, HEADS * HEAD), 1.0, 6.0, ((0, 16), (1, 2)))
    learning_strength_preacts = centred(splits[4], (2, TOKENS, HEADS), 1.5, 6.0, ((1, 16), (2, 2)), jnp.float32)
    forget_preacts = draw_forget_preacts(jax.random.fold_in(splits[14], 71), 0)
    forgetting_speed_exponent = draw_forgetting_speed_exponent(jax.random.fold_in(splits[14], 71), 0)
    extra_forgetting_spikes = draw_extra_forgetting_spikes(jax.random.fold_in(splits[14], 71), 0)
    sample_membership = jnp.searchsorted(jnp.cumsum(ragged_sizes(splits[8], DOCS, TOKENS, DOC_MOST, 1)), jnp.arange(TOKENS), side="right").astype(jnp.int32)
    channel_group_scaling = jnp.clip(1.0 + 0.18 * jax.random.normal(splits[9], (HEAD,), jnp.float32), 0.1, 1.9)
    blend_exit_weights = centred(splits[10], (HEADS * HEAD, D), (HEADS * HEAD) ** -0.5, 0.1875, ((0, 2),))
    dense_block_scaling = jnp.clip(1.0 + 0.18 * jax.random.normal(splits[11], (D,), jnp.float32), 0.1, 1.9)
    widen_projection_weights = centred(splits[12], (D, FF), D ** -0.5, 0.125, ((0, 16), (1, 2)))
    shrink_projection_weights = centred(splits[13], (FF, D), FF ** -0.5, 0.0625, ((0, 2), (1, 16)))
    return {"skip_path_inputs": skip_path_inputs, "probe_vectors": probe_vectors, "lookup_vectors": lookup_vectors, "payload_vectors": payload_vectors, "learning_strength_preacts": learning_strength_preacts, "forget_preacts": forget_preacts, "forgetting_speed_exponent": forgetting_speed_exponent, "extra_forgetting_spikes": extra_forgetting_spikes, "sample_membership": sample_membership, "channel_group_scaling": channel_group_scaling, "blend_exit_weights": blend_exit_weights, "dense_block_scaling": dense_block_scaling, "widen_projection_weights": widen_projection_weights, "shrink_projection_weights": shrink_projection_weights}


HIGH = lax.Precision.HIGHEST
EPSILON = 1e-06

def block_pass(memory, probe_vectors, lookup_vectors, payload_vectors, strengths, forget_multipliers, doc_ids, prior_doc, wanted):
    value_width = payload_vectors.shape[-1]
    block_len = probe_vectors.shape[1]
    running = jnp.cumsum(forget_multipliers, axis=-1)
    row_ids = lax.broadcasted_iota(jnp.int32, (block_len, block_len), 0)
    col_ids = lax.broadcasted_iota(jnp.int32, (block_len, block_len), 1)
    shared = doc_ids[:, None] == doc_ids[None, :]
    within = (row_ids >= col_ids) & shared
    before = (row_ids > col_ids) & shared
    spread = jnp.exp(jnp.where(within, running[:, :, None] - running[:, None, :], -jnp.inf))
    linked = (doc_ids == prior_doc).astype(jnp.float32)
    ending = (doc_ids == doc_ids[-1]).astype(jnp.float32)
    weighted = lookup_vectors * strengths[..., None]
    system = jnp.eye(block_len, dtype=jnp.float32) + jnp.where(before, jnp.einsum('hik,hjk->hij', weighted, lookup_vectors, precision=HIGH) * spread, 0.0)
    right_side = jnp.concatenate([payload_vectors * strengths[..., None], weighted * (jnp.exp(running) * linked)[..., None]], axis=-1)
    solved = jax.scipy.linalg.solve_triangular(system, right_side, lower=True, unit_diagonal=True)
    update = solved[..., :value_width] - jnp.einsum('hck,hkw->hcw', solved[..., value_width:], memory, precision=HIGH)
    faded_keys = lookup_vectors * (jnp.exp(running[:, -1:] - running) * ending)[..., None]
    kept_share = jnp.exp(running[:, -1]) * linked[-1]
    renewed = memory * kept_share[:, None, None] + jnp.einsum('hck,hcw->hkw', faded_keys, update, precision=HIGH)
    if not wanted:
        return (renewed, None)
    scores = jnp.where(within, jnp.einsum('hik,hjk->hij', probe_vectors, lookup_vectors, precision=HIGH) * spread, 0.0)
    reading = jnp.einsum('hck,hkw->hcw', probe_vectors * (jnp.exp(running) * linked)[..., None], memory, precision=HIGH)
    return (renewed, reading + jnp.einsum('hij,hjw->hiw', scores, update, precision=HIGH))

def run_blocks(memory, prior_doc, probe_vectors, lookup_vectors, payload_vectors, strengths, forget_multipliers, doc_ids, wanted):
    head_count, length, key_width = probe_vectors.shape
    block_count = length // BLOCK

    def split_blocks(tensor):
        return jnp.moveaxis(tensor.reshape((head_count, block_count, BLOCK) + tensor.shape[2:]), 1, 0)

    def advance(carried, inputs):
        held, earlier_doc = carried
        query_block, key_block, value_block, gate_block, decay_block, doc_block = inputs
        held, produced = block_pass(held, query_block, key_block, value_block, gate_block, decay_block, doc_block, earlier_doc, wanted)
        return ((held, doc_block[-1]), produced)
    (final, _), produced = lax.scan(advance, (memory, prior_doc), (split_blocks(probe_vectors), split_blocks(lookup_vectors), split_blocks(payload_vectors), split_blocks(strengths), split_blocks(forget_multipliers), doc_ids.reshape(block_count, BLOCK)))
    if wanted:
        produced = jnp.moveaxis(produced, 0, 1).reshape(head_count, length, -1)
    return (final, produced)

def unit_rows(tensor):
    return tensor * lax.rsqrt(lax.optimization_barrier(jnp.sum(tensor * tensor, axis=-1, keepdims=True)) + EPSILON)

def heads_first(tensor):
    row_count = tensor.shape[0]
    return jnp.transpose(tensor.astype(jnp.float32).reshape(row_count, HEADS, HEAD), (1, 0, 2))

def sweep(probe_vectors, lookup_vectors, payload_vectors, strengths, forget_multipliers, doc_ids):
    start_state = jnp.zeros((probe_vectors.shape[0], HEAD, HEAD), jnp.float32)
    _, produced = run_blocks(start_state, jnp.full((), -1, jnp.int32), probe_vectors, lookup_vectors, payload_vectors, strengths, forget_multipliers, doc_ids, True)
    return produced

def reference(skip_path_inputs, probe_vectors, lookup_vectors, payload_vectors, learning_strength_preacts, forget_preacts, forgetting_speed_exponent, extra_forgetting_spikes, sample_membership, channel_group_scaling, blend_exit_weights, dense_block_scaling, widen_projection_weights, shrink_projection_weights):
    length = probe_vectors.shape[0]
    query_heads = unit_rows(heads_first(probe_vectors)) * HEAD ** (-0.5)
    key_heads = unit_rows(heads_first(lookup_vectors))
    value_heads = heads_first(payload_vectors)
    strengths = jnp.transpose(jax.nn.sigmoid(learning_strength_preacts), (0, 2, 1))
    forget_multipliers = jnp.transpose(-jnp.exp(forgetting_speed_exponent)[:, None, :] * jax.nn.softplus(forget_preacts) + extra_forgetting_spikes, (0, 2, 1))
    forward_out = sweep(query_heads, key_heads, value_heads, strengths[0], forget_multipliers[0], sample_membership)
    backward_out = sweep(jnp.flip(query_heads, 1), jnp.flip(key_heads, 1), jnp.flip(value_heads, 1), jnp.flip(strengths[1], 1), jnp.flip(forget_multipliers[1], 1), jnp.flip(sample_membership, 0))
    attn = forward_out + jnp.flip(backward_out, 1)
    scaled = attn * lax.rsqrt(lax.optimization_barrier(jnp.mean(attn * attn, axis=-1, keepdims=True)) + EPSILON) * channel_group_scaling
    mixed = jnp.transpose(scaled, (1, 0, 2)).reshape(length, HEADS * HEAD).astype(jnp.bfloat16)
    group_width = HEADS * HEAD // N_TP
    projected = jnp.zeros((length, D), jnp.float32)
    for member in range(N_TP):
        group_term = jnp.dot(mixed[:, member * group_width:(member + 1) * group_width].astype(jnp.float32), blend_exit_weights[member * group_width:(member + 1) * group_width].astype(jnp.float32), preferred_element_type=jnp.float32)
        projected = projected + lax.optimization_barrier(group_term.astype(jnp.bfloat16)).astype(jnp.float32)
    residual = skip_path_inputs.astype(jnp.float32) + projected
    normed = (residual * lax.rsqrt(lax.optimization_barrier(jnp.mean(residual * residual, axis=-1, keepdims=True)) + EPSILON) * dense_block_scaling).astype(jnp.bfloat16)
    unit_width = FF // N_TP
    lowered = jnp.zeros((length, D), jnp.float32)
    for member in range(N_TP):
        raised = jnp.dot(normed.astype(jnp.float32), widen_projection_weights[:, member * unit_width:(member + 1) * unit_width].astype(jnp.float32), preferred_element_type=jnp.float32)
        active = jnp.square(jax.nn.relu(raised)).astype(jnp.bfloat16)
        group_term = jnp.dot(active.astype(jnp.float32), shrink_projection_weights[member * unit_width:(member + 1) * unit_width].astype(jnp.float32), preferred_element_type=jnp.float32)
        lowered = lowered + lax.optimization_barrier(group_term.astype(jnp.bfloat16)).astype(jnp.float32)
    return (residual + lowered).astype(jnp.bfloat16)
```

```python
import functools

import jax
import jax.numpy as jnp
from jax import lax
from jax.experimental import pallas as pl
from jax.experimental.pallas import tpu as pltpu
from jax.sharding import PartitionSpec as P

EPSILON = 1e-06
F32 = jnp.float32
BF16 = jnp.bfloat16
MESH = pl.DeviceIdType.MESH


def mm(a, b, dims=((1,), (0,))):
    return lax.dot_general(
        a.astype(BF16), b.astype(BF16), (dims, ((), ())), preferred_element_type=F32
    )


def exact_mm(a, b, dims=((1,), (0,))):
    return lax.dot_general(
        a, b, (dims, ((), ())), precision=lax.Precision.HIGHEST, preferred_element_type=F32
    )


def mixer_kernel(
    n_sp,
    group,
    width,
    q_ref,
    k_ref,
    v_ref,
    beta_ref,
    g_ref,
    gt_ref,
    doc_col_ref,
    doc_row_ref,
    join_ref,
    w1_ref,
    w2_ref,
    attn,
    reads,
    maps,
    w1g_ref,
    w2g_ref,
    w_send,
    w_recv,
    own_sem,
):
    me = lax.axis_index("sp")
    rows = q_ref.shape[0]
    heads = q_ref.shape[1] // width
    part = w1_ref.shape[1] // group
    depth = w1_ref.shape[0]

    barrier = pltpu.get_barrier_semaphore()

    def greet(d, carry):
        pl.semaphore_signal(
            barrier, inc=1, device_id={"sp": lax.rem(me + d, n_sp)}, device_id_type=MESH
        )
        return carry

    lax.fori_loop(1, n_sp, greet, 0)
    pl.semaphore_wait(barrier, n_sp - 1)

    def weight_copies(d):
        to = lax.rem(me + d, n_sp)
        at = pl.multiple_of(lax.rem(to, group) * part, part)
        wide = pltpu.make_async_remote_copy(
            src_ref=w1_ref.at[:, pl.ds(at, part)],
            dst_ref=w1g_ref.at[pl.ds(pl.multiple_of(me * depth, depth), depth), :],
            send_sem=w_send.at[0, d],
            recv_sem=w_recv.at[0, d],
            device_id={"sp": to},
            device_id_type=MESH,
        )
        shrink = pltpu.make_async_remote_copy(
            src_ref=w2_ref.at[pl.ds(at, part), :],
            dst_ref=w2g_ref.at[me],
            send_sem=w_send.at[1, d],
            recv_sem=w_recv.at[1, d],
            device_id={"sp": to},
            device_id_type=MESH,
        )
        return wide, shrink

    def send_weights(d, carry):
        for copy in weight_copies(d):
            copy.start()
        return carry

    here = pl.multiple_of(lax.rem(me, group) * part, part)
    own_wide = pltpu.make_async_copy(
        w1_ref.at[:, pl.ds(here, part)],
        w1g_ref.at[pl.ds(pl.multiple_of(me * depth, depth), depth), :],
        own_sem.at[0],
    )
    own_shrink = pltpu.make_async_copy(
        w2_ref.at[pl.ds(here, part), :], w2g_ref.at[me], own_sem.at[1]
    )
    lax.fori_loop(1, n_sp, send_weights, 0)
    own_wide.start()
    own_shrink.start()

    row_ids = lax.broadcasted_iota(jnp.int32, (rows, rows), 0)
    col_ids = lax.broadcasted_iota(jnp.int32, (rows, rows), 1)
    doc_col = doc_col_ref[...]
    doc_row = doc_row_ref[...]
    shared = doc_col == doc_row
    eye = (row_ids == col_ids).astype(F32)
    lower = (row_ids >= col_ids).astype(F32)
    upper = (row_ids <= col_ids).astype(F32)
    g = g_ref[...]
    gt = gt_ref[...]
    run_cols = (exact_mm(lower, g), exact_mm(upper, g))
    run_rows = (exact_mm(gt, upper), exact_mm(gt, lower))
    first = doc_col[0:1, :]
    last = doc_col[rows - 1 : rows, :]
    from_first = (doc_col == first).astype(F32)
    from_last = (doc_col == last).astype(F32)
    whole = (first == last).astype(F32)
    levels = []
    size = 1
    while size < rows:
        levels.append(
            (row_ids // (2 * size) == col_ids // (2 * size)) & (row_ids // size != col_ids // size)
        )
        size *= 2

    for h in range(heads):
        cols = slice(h * width, (h + 1) * width)
        q = q_ref[:, cols].astype(F32)
        k = k_ref[:, cols].astype(F32)
        v = v_ref[:, cols].astype(F32)
        q = q * lax.rsqrt(jnp.sum(q * q, axis=1, keepdims=True) + EPSILON) * width ** (-0.5)
        k = k * lax.rsqrt(jnp.sum(k * k, axis=1, keepdims=True) + EPSILON)
        keys = mm(k, k, ((1,), (1,)))
        probes = mm(q, k, ((1,), (1,)))
        total = None
        for w in range(2):
            u = w * heads + h
            run = run_cols[w][:, u : u + 1]
            gap = run - run_rows[w][u : u + 1, :]
            within = ((row_ids >= col_ids) if w == 0 else (row_ids <= col_ids)) & shared
            spread = jnp.where(within, jnp.exp(jnp.where(within, gap, 0.0)), 0.0)
            beta = beta_ref[:, u : u + 1]
            system = jnp.where(row_ids == col_ids, 0.0, keys * spread * beta)
            inverse = eye - jnp.where(levels[0], system, 0.0)
            for level in levels[1:]:
                inverse = inverse - mm(inverse, mm(jnp.where(level, system, 0.0), inverse))
            link = from_first if w == 0 else from_last
            ending = from_last if w == 0 else from_first
            fade = jnp.exp(run) * link
            right = jnp.concatenate([v * beta, k * (beta * fade)], axis=1)
            solved = mm(inverse, right)
            end = run[rows - 1 : rows, :] if w == 0 else run[0:1, :]
            faded = k * (jnp.exp(end - run) * ending)
            moved = mm(solved, faded, ((0,), (0,)))
            kept = jnp.exp(end) * whole
            join = join_ref[w : w + 1, :]
            maps[u, :width, :] = ((eye * kept - moved[width:, :]) * join).astype(BF16)
            maps[u, width:, :] = moved[:width, :].astype(BF16)
            scored = mm(probes * spread, solved)
            reads[u] = ((q * fade - scored[:, width:]) * join).astype(BF16)
            total = scored[:, :width] if w == 0 else total + scored[:, :width]
        attn[h] = total

    def weights_done(d, carry):
        for copy in weight_copies(d):
            copy.wait()
        return carry

    lax.fori_loop(1, n_sp, weights_done, 0)
    own_wide.wait()
    own_shrink.wait()


def finish_kernel(n_sp, attn, reads, gathered, gain_ref, mixed_ref, held):
    me = lax.axis_index("sp")
    units, _, width = reads.shape
    heads = units // 2

    held[...] = jnp.zeros_like(held)

    def hop_of(backward):
        def hop(n, carry):
            s = n_sp - 1 - n if backward else n
            for u in range(backward * heads, backward * heads + heads):
                held[u] = mm(held[u], gathered[s, u, :width, :]) + gathered[
                    s, u, width:, :
                ].astype(F32)
            return carry

        return hop

    lax.fori_loop(0, me, hop_of(0), 0)
    lax.fori_loop(0, n_sp - 1 - me, hop_of(1), 0)
    for h in range(heads):
        total = attn[h]
        for u in (h, heads + h):
            total = total + mm(reads[u], held[u], ((1,), (1,)))
        scaled = (
            total
            * lax.rsqrt(jnp.mean(total * total, axis=1, keepdims=True) + EPSILON)
            * gain_ref[...]
        )
        mixed_ref[:, h * width : (h + 1) * width] = scaled.astype(BF16)


def dense_kernel(
    n_tp,
    group,
    tile,
    x_ref,
    res_ref,
    w1_ref,
    w2_ref,
    out_ref,
    held,
    total,
    terms,
    landed,
    x_send,
    x_recv,
    p_send,
    p_recv,
):
    me = lax.axis_index("sp")
    core = lax.axis_index("tp")
    base = me // group * group
    place = me - base
    rows = x_ref.shape[0]
    part = w1_ref.shape[1]
    cols = out_ref.shape[1]

    barrier = pltpu.get_barrier_semaphore()
    for d in range(group):
        for e in range(n_tp):
            if d or e:
                pl.semaphore_signal(
                    barrier,
                    inc=1,
                    device_id={
                        "sp": base + lax.rem(place + d, group),
                        "tp": lax.rem(core + e, n_tp),
                    },
                    device_id_type=MESH,
                )
    pl.semaphore_wait(barrier, group * n_tp - 1)

    def x_copy(d):
        return pltpu.make_async_remote_copy(
            src_ref=x_ref,
            dst_ref=held.at[d],
            send_sem=x_send.at[d],
            recv_sem=x_recv.at[d],
            device_id={"sp": base + lax.rem(place + d, group)},
            device_id_type=MESH,
        )

    def p_copy(d, e):
        to = lax.rem(core + e, n_tp)
        return pltpu.make_async_remote_copy(
            src_ref=terms.at[d, to],
            dst_ref=landed.at[d, e],
            send_sem=p_send.at[d * n_tp + e],
            recv_sem=p_recv.at[d * n_tp + e],
            device_id={"sp": base + lax.rem(place - d + group, group), "tp": to},
            device_id_type=MESH,
        )

    for d in range(1, group):
        x_copy(d).start()

    held[0] = x_ref[...]
    for d in range(group):
        if d:
            x_copy(d).wait_recv()

        def step(i, carry):
            at = pl.multiple_of(i * tile, tile)
            raised = jnp.dot(
                held[d], w1_ref[:, pl.ds(at, tile)], preferred_element_type=F32
            )
            active = jnp.square(jnp.maximum(raised, 0.0)).astype(BF16)
            total[...] += jnp.dot(active, w2_ref[pl.ds(at, tile), :], preferred_element_type=F32)
            return carry

        total[...] = jnp.zeros_like(total)
        lax.fori_loop(0, part // tile, step, 0)
        for t in range(n_tp):
            terms[d, t] = total[:, t * cols : (t + 1) * cols].astype(BF16)
        for e in range(n_tp):
            if d or e:
                p_copy(d, e).start()

    summed = res_ref[...] + terms[0, core].astype(F32)
    for d in range(group):
        for e in range(n_tp):
            if d or e:
                p_copy(d, e).wait_recv()
                summed = summed + landed[d, e].astype(F32)
    out_ref[...] = summed.astype(out_ref.dtype)
    for d in range(1, group):
        x_copy(d).wait_send()
    for d in range(group):
        for e in range(n_tp):
            if d or e:
                p_copy(d, e).wait_send()


def shards(
    skip_path_inputs,
    probe_vectors,
    lookup_vectors,
    payload_vectors,
    learning_strength_preacts,
    forget_preacts,
    forgetting_speed_exponent,
    extra_forgetting_spikes,
    sample_membership,
    channel_group_scaling,
    blend_exit_weights,
    dense_block_scaling,
    widen_projection_weights,
    shrink_projection_weights,
):
    n_sp, n_tp = lax.axis_size("sp"), lax.axis_size("tp")
    me = lax.axis_index("sp")
    rows = probe_vectors.shape[0]
    width = channel_group_scaling.shape[0]
    heads = probe_vectors.shape[1] // width
    units = 2 * heads
    model_width = skip_path_inputs.shape[1]
    depth, hidden = widen_projection_weights.shape
    out_cols = shrink_projection_weights.shape[1]
    group = 4
    part = hidden // group

    beta = jax.nn.sigmoid(learning_strength_preacts)
    decay = (
        -jnp.exp(forgetting_speed_exponent)[:, None, :] * jax.nn.softplus(forget_preacts)
        + extra_forgetting_spikes
    )
    side = lambda a: jnp.transpose(a, (1, 0, 2)).reshape(rows, units)
    beta, decay = side(beta), side(decay)
    earlier = lax.ppermute(sample_membership[-1:], "sp", [(i, i + 1) for i in range(n_sp - 1)])
    later = lax.ppermute(sample_membership[:1], "sp", [(i + 1, i) for i in range(n_sp - 1)])
    joined = jnp.stack(
        [
            (earlier == sample_membership[:1]) & (me > 0),
            (later == sample_membership[-1:]) & (me < n_sp - 1),
        ]
    ).astype(F32)
    joined = jnp.broadcast_to(joined, (2, width))

    vmem = pl.BlockSpec(memory_space=pltpu.VMEM)
    anywhere = pl.BlockSpec(memory_space=pl.ANY)
    dma = pltpu.SemaphoreType.DMA
    attn, reads, maps, wide, shrink = pl.pallas_call(
        functools.partial(mixer_kernel, n_sp, group, width),
        out_shape=(
            jax.ShapeDtypeStruct((heads, rows, width), F32),
            jax.ShapeDtypeStruct((units, rows, width), BF16),
            jax.ShapeDtypeStruct((units, 2 * width, width), BF16),
            jax.ShapeDtypeStruct((depth * n_sp, part), BF16),
            jax.ShapeDtypeStruct((n_sp, part, out_cols), BF16),
        ),
        in_specs=[vmem] * 11,
        out_specs=(vmem, vmem, vmem, anywhere, anywhere),
        scratch_shapes=[
            dma((2, n_sp)),
            dma((2, n_sp)),
            dma((2,)),
        ],
        compiler_params=pltpu.CompilerParams(
            collective_id=0, has_side_effects=True, vmem_limit_bytes=40 * 1024 * 1024
        ),
        name="mixer",
    )(
        probe_vectors,
        lookup_vectors,
        payload_vectors,
        beta,
        decay,
        decay.T,
        sample_membership[:, None],
        sample_membership[None, :],
        joined,
        widen_projection_weights,
        shrink_projection_weights,
    )
    mixed = pl.pallas_call(
        functools.partial(finish_kernel, n_sp),
        out_shape=jax.ShapeDtypeStruct((rows, heads * width), BF16),
        in_specs=[vmem] * 4,
        out_specs=vmem,
        scratch_shapes=[pltpu.VMEM((units, width, width), F32)],
        compiler_params=pltpu.CompilerParams(vmem_limit_bytes=40 * 1024 * 1024),
        name="finish",
    )(attn, reads, lax.all_gather(maps, "sp"), channel_group_scaling[None, :])
    shrink = jnp.transpose(shrink, (1, 0, 2)).reshape(part, n_sp * out_cols)

    head_terms = jnp.dot(mixed, blend_exit_weights, preferred_element_type=F32).astype(BF16)
    col_count = model_width // n_tp
    col_start = lax.axis_index("tp") * col_count
    residual = skip_path_inputs.astype(F32) + lax.psum(head_terms, "tp").astype(F32)
    normed = (
        residual
        * lax.rsqrt(jnp.mean(residual * residual, axis=1, keepdims=True) + EPSILON)
        * dense_block_scaling
    ).astype(BF16)
    own_residual = lax.dynamic_slice_in_dim(residual, col_start, col_count, 1)
    return pl.pallas_call(
        functools.partial(dense_kernel, n_tp, group, min(part, 256)),
        out_shape=jax.ShapeDtypeStruct((rows, col_count), BF16),
        in_specs=[vmem] * 4,
        out_specs=vmem,
        scratch_shapes=[
            pltpu.VMEM((group, rows, model_width), BF16),
            pltpu.VMEM((rows, model_width), F32),
            pltpu.VMEM((group, n_tp, rows, col_count), BF16),
            pltpu.VMEM((group, n_tp, rows, col_count), BF16),
            dma((group,)),
            dma((group,)),
            dma((group * n_tp,)),
            dma((group * n_tp,)),
        ],
        compiler_params=pltpu.CompilerParams(
            collective_id=1, has_side_effects=True, vmem_limit_bytes=48 * 1024 * 1024
        ),
        name="dense",
    )(normed, own_residual, wide, shrink)


def solution(mesh):
    placed = (
        P("sp", None),
        P("sp", "tp"),
        P("sp", "tp"),
        P("sp", "tp"),
        P(None, "sp", "tp"),
        P(None, "sp", "tp"),
        P(None, "tp"),
        P(None, "sp", "tp"),
        P("sp"),
        P(),
        P("tp", None),
        P(),
        P("sp", "tp"),
        P("tp", "sp"),
    )
    return jax.shard_map(
        shards, mesh=mesh, in_specs=placed, out_specs=P("sp", "tp"), check_vma=False
    )
```
